32 devices in a mesh: sp: 4 (over z), fs: 4 (over y, x), tp: 2 (over core).
Axes of the slice: x: 2, y: 2, z: 4, core: 2. Of those that a mesh axis runs over, the one named last changes fastest.
Arguments:
- inputs: bfloat16 [16384, 2048], P(('fs', 'sp'), 'tp'), parts along dimension 0, may hold values from -270 to 270
- mix_gain: float32 [2048], replicated, may hold values from 0.1 to 1.9
- w_query: bfloat16 [2048, 1024], P(None, 'tp'), may hold values from -0.125 to 0.125
- w_key: bfloat16 [2048, 256], P(None, 'tp'), may hold values from -0.125 to 0.125
- w_value: bfloat16 [2048, 256], P(None, 'tp'), may hold values from -0.125 to 0.125
- query_gain: float32 [64], replicated, may hold values from 0 to 14, as said below
- key_gain: float32 [64], replicated, may hold values from 0 to 14, as said below
- sink_logit: float32 [16], P('tp'), may hold values from 3 to 7
- w_inner: bfloat16 [2048, 1024], P(None, 'tp'), may hold values from -0.125 to 0.125
- w_bmat: bfloat16 [2048, 512], P(None, 'tp'), may hold values from -0.125 to 0.125
- w_cmat: bfloat16 [2048, 512], P(None, 'tp'), may hold values from -0.125 to 0.125
- w_gate: bfloat16 [2048, 1024], P(None, 'tp'), may hold values from -0.125 to 0.125
- w_step: bfloat16 [2048, 2, 16], P(None, None, 'tp'), may hold values from -0.125 to 0.125
- conv_inner: bfloat16 [5, 1024], P(None, 'tp'), may hold values from -2.5 to 2.5
- conv_bmat: bfloat16 [5, 512], P(None, 'tp'), may hold values from -2.5 to 2.5
- conv_cmat: bfloat16 [5, 512], P(None, 'tp'), may hold values from -2.5 to 2.5
- step_bias: float32 [2, 16], P(None, 'tp'), may hold values from -1 to 1
- decay_rate: float32 [2, 16], P(None, 'tp'), may hold values from 0 to 1, as said below
- decay_offset: float32 [4096, 2, 16], P('sp', None, 'tp'), may hold values from -3 to 0, as said below
- start_state: float32 [8, 16, 64, 128], P('fs', 'tp'), parts along dimension 0, may hold values from -96 to 96
- group_gain: float32 [1024], P('tp'), may hold values from 0.1 to 1.9
- w_out_attn: bfloat16 [1024, 2048], P('tp'), may hold values from -1.5 to 1.5
- w_out_state: bfloat16 [1024, 2048], P('tp'), may hold values from -0.1875 to 0.1875
Outputs:
- mixed: bfloat16 [16384, 2048], P(('fs', 'sp', 'tp')), parts along dimension 0
The draws below stay inside these ranges and needn't reach their ends.
There are 4 independent parts, one for each index of `fs`. The reference program is written for one: setup_inputs(seed, part) draws one part's arguments, and reference() takes and returns one part's arrays. A program takes and returns all parts, laid end to end along the dimension named above; an argument that names none is the same for every part. Nothing has to cross between parts.
Inputs may be any that keep to these rules, and one draw needn't show every extreme that they name: `query_gain`: positive. `key_gain`: positive. `decay_rate`: positive. `decay_offset`: never positive.
All inputs are finite; a program needn't handle non-finite values.
Results may differ from the reference program's by a relative error of at most 0.035.
Values may be sent and summed in bfloat16 or wider, within the bound.
A program may use at most 128 MiB of HBM per device.

```python
import math
import jax
import jax.numpy as jnp
from jax import lax

D = 2048
HEAD = 64
A_HEADS = 16
A_KV = 4
MIXER_HEADS = 16
S_GROUPS = 4
STATE = 128
CONV = 5
WINDOW = 128
STATE_BLOCK = 128
TOK_DEV = 1024
SEQUENCE_LENGTH = 4096
S_INNER = 1024
N_TP = 2


def draw_inputs(key, part):
    base_key = jax.random.fold_in(key, 11)
    noise_key, row_key, column_key = jax.random.split(base_key, 3)
    row_scale = jnp.exp(jax.random.uniform(row_key, (SEQUENCE_LENGTH, 1), jnp.float32, 0.0, math.log(10.0)))
    column_ramp = jnp.exp(math.log(4.0) * jnp.arange(D, dtype=jnp.float32) / D)
    column_scale = column_ramp[None, :] * jnp.exp(jax.random.uniform(column_key, (1, D), jnp.float32, -0.5, 0.5))
    values = jnp.clip(jax.random.normal(noise_key, (SEQUENCE_LENGTH, D), jnp.float32), -4.0, 4.0)
    return (values * row_scale * column_scale).astype(jnp.bfloat16)


def gain_table(key, salt):
    gain_key = jax.random.fold_in(key, salt)
    return jax.random.uniform(gain_key, (HEAD,), jnp.float32, 0.5, 1.5)


def draw_query_gain(key, part):
    return gain_table(key, 21)


def draw_key_gain(key, part):
    return gain_table(key, 22)


def slow_heads(key):
    ranking = jax.random.permutation(jax.random.fold_in(key, 31), 2 * MIXER_HEADS)
    kept_count = MIXER_HEADS
    return (ranking < kept_count).reshape(2, MIXER_HEADS)


def base_rates(key):
    slowly = slow_heads(key)
    quick_rates = jax.random.uniform(jax.random.fold_in(key, 41), (2, MIXER_HEADS), jnp.float32, 1.5, 2.5) / STATE_BLOCK
    return jnp.where(slowly, 0.2 / SEQUENCE_LENGTH, quick_rates)


def draw_decay_rate(key, part):
    return base_rates(key)


def draw_decay_offset(key, part):
    rates = base_rates(key)
    device_blocks = SEQUENCE_LENGTH // TOK_DEV
    factor_key, position_random_key, level_random_key = jax.random.split(jax.random.fold_in(key, 51), 3)
    factors = jnp.exp(jax.random.uniform(factor_key, (device_blocks, 1, 2, MIXER_HEADS), jnp.float32, math.log(0.5), math.log(2.5)))
    constant_level = -jnp.broadcast_to(factors * rates, (device_blocks, TOK_DEV, 2, MIXER_HEADS)).reshape(SEQUENCE_LENGTH, 2, MIXER_HEADS)
    spike_position = jax.random.randint(position_random_key, (2, 2, MIXER_HEADS), 0, SEQUENCE_LENGTH)
    spike_level = jnp.log(jax.random.uniform(level_random_key, (2, 2, MIXER_HEADS), jnp.float32, 0.5, 0.8))
    spike_mask = jnp.arange(SEQUENCE_LENGTH)[:, None, None, None] == spike_position[None]
    spike_count = jnp.sum(jnp.where(spike_mask, spike_level[None], 0.0), axis=1)
    return constant_level + spike_count


def levels(key, extent, cuts, least, high):
    loudness, own = 1.0, jax.random.fold_in(key, 6)
    for dim, shards_of in cuts:
        draws = jnp.exp(jax.random.uniform(jax.random.fold_in(own, dim), (shards_of,), jnp.float32, least / len(cuts), high / len(cuts)))
        loudness = loudness * jnp.repeat(draws, extent[dim] // shards_of).reshape([-1 if axis == dim else 1 for axis in range(len(extent))])
    return loudness


def bell_draw(stream_key, extent, scale, reach, cuts=(), kind=jnp.bfloat16):
    result = jax.random.normal(stream_key, extent, jnp.float32) * scale
    if len(cuts) > 0:
        result = levels(stream_key, extent, cuts, -0.22, 0.18) * result
    return jnp.clip(result, min=-reach, max=reach).astype(kind)


def setup_inputs(seed: int = 0, part: int = 0) -> dict:
    splits = jax.random.split(jax.random.key(seed), 24)
    own_keys = jax.random.split(jax.random.fold_in(splits[23], part), 24)
    inputs = draw_inputs(jax.random.fold_in(jax.random.fold_in(splits[23], part), 71), part)
    mix_gain = jnp.clip(1.0 + 0.18 * jax.random.normal(splits[1], (D,), jnp.float32), 0.1, 1.9)
    w_query = bell_draw(splits[2], (D, A_HEADS * HEAD), D ** -0.5, 0.125, ((1, 2),))
    w_key = bell_draw(splits[3], (D, A_KV * HEAD), D ** -0.5, 0.125, ((1, 2),))
    w_value = bell_draw(splits[4], (D, A_KV * HEAD), D ** -0.5, 0.125, ((1, 2),))
    query_gain = draw_query_gain(jax.random.fold_in(splits[23], 71), part)
    key_gain = draw_key_gain(jax.random.fold_in(splits[23], 71), part)
    sink_logit = jnp.clip(3.0 + 4.0 * jax.random.uniform(splits[7], (A_HEADS,), jnp.float32) ** levels(splits[7], (A_HEADS,), ((0, 2),), -0.2, 0.2), 3.0, 7.0)
    w_inner = bell_draw(splits[8], (D, S_INNER), D ** -0.5, 0.125, ((1, 2),))
    w_bmat = bell_draw(splits[9], (D, S_GROUPS * STATE), D ** -0.5, 0.125, ((1, 2),))
    w_cmat = bell_draw(splits[10], (D, S_GROUPS * STATE), D ** -0.5, 0.125, ((1, 2),))
    w_gate = bell_draw(splits[11], (D, S_INNER), D ** -0.5, 0.125, ((1, 2),))
    w_step = bell_draw(splits[12], (D, 2, MIXER_HEADS), D ** -0.5, 0.125, ((2, 2),))
    conv_inner = bell_draw(splits[13], (CONV, S_INNER), CONV ** -0.5, 2.5, ((1, 2),))
    conv_bmat = bell_draw(splits[14], (CONV, S_GROUPS * STATE), CONV ** -0.5, 2.5, ((1, 2),))
    conv_cmat = bell_draw(splits[15], (CONV, S_GROUPS * STATE), CONV ** -0.5, 2.5, ((1, 2),))
    step_bias = jnp.clip(jax.random.uniform(splits[16], (2, MIXER_HEADS), jnp.float32, -1.0, 1.0) * levels(splits[16], (2, MIXER_HEADS), ((1, 2),), -0.4, 0.0), -1.0, 1.0)
    decay_rate = draw_decay_rate(jax.random.fold_in(splits[23], 71), part)
    decay_offset = draw_decay_offset(jax.random.fold_in(splits[23], 71), part)
    start_state = bell_draw(own_keys[19], (2, MIXER_HEADS, HEAD, STATE), (SEQUENCE_LENGTH ** 0.5 // 4), 96.0, ((1, 2),), jnp.float32)
    group_gain = jnp.clip(1.0 + 0.18 * jax.random.normal(splits[20], (S_INNER,), jnp.float32), 0.1, 1.9)
    w_out_attn = bell_draw(splits[21], (A_HEADS * HEAD, D), (A_HEADS * HEAD // 64) ** -0.5, 1.5, ((0, 2),))
    w_out_state = bell_draw(splits[22], (S_INNER, D), S_INNER ** -0.5, 0.1875, ((0, 2),))
    return dict(inputs=inputs, mix_gain=mix_gain, w_query=w_query, w_key=w_key, w_value=w_value, query_gain=query_gain, key_gain=key_gain, sink_logit=sink_logit, w_inner=w_inner, w_bmat=w_bmat, w_cmat=w_cmat, w_gate=w_gate, w_step=w_step, conv_inner=conv_inner, conv_bmat=conv_bmat, conv_cmat=conv_cmat, step_bias=step_bias, decay_rate=decay_rate, decay_offset=decay_offset, start_state=start_state, group_gain=group_gain, w_out_attn=w_out_attn, w_out_state=w_out_state)


epsilon = 1e-06
rotary_base = 10000.0

def head_norm(values, gain):
    return values * lax.rsqrt(lax.optimization_barrier(jnp.mean(values * values, axis=-1, keepdims=True)) + epsilon) * gain

def rotate(values, positions):
    half_dim = values.shape[-1] // 2
    frequency = rotary_base ** (-jnp.arange(half_dim, dtype=jnp.float32) / half_dim)
    angles = positions.astype(jnp.float32)[:, None] * frequency[None, :]
    shaped = (angles.shape[0],) + (1,) * (values.ndim - 2) + (half_dim,)
    cosine = jnp.cos(angles).reshape(shaped)
    sine_table = jnp.sin(angles).reshape(shaped)
    first_half = values[..., :half_dim]
    second_half = values[..., half_dim:]
    return jnp.concatenate([first_half * cosine - second_half * sine_table, second_half * cosine + first_half * sine_table], axis=-1)

def attend_block(queries, keys, values, sink_logit, key_pos, length):
    scores = jnp.einsum('qhgd,khd->hgqk', queries.astype(jnp.float32), keys.astype(jnp.float32)) * HEAD ** (-0.5)
    offsets = jnp.arange(3 * WINDOW) - WINDOW
    nearby = jnp.abs(offsets[None, :] - jnp.arange(WINDOW)[:, None]) <= WINDOW
    inside = (key_pos >= 0) & (key_pos < length)
    allowed = nearby & inside[None, :]
    masked = jnp.where(allowed, scores, -jnp.inf)
    highest = jnp.maximum(lax.optimization_barrier(jnp.max(masked, axis=-1, keepdims=True)), sink_logit[:, :, None, None])
    raised = jnp.exp(masked - highest)
    denominator = jnp.exp(sink_logit[:, :, None, None] - highest) + lax.optimization_barrier(jnp.sum(raised, axis=-1, keepdims=True))
    weights = (raised / denominator).astype(jnp.bfloat16)
    return jnp.einsum('hgqk,khe->qhge', weights.astype(jnp.float32), values.astype(jnp.float32)).astype(jnp.bfloat16)

def ssd_blocks(inner_act, bmat_act, cmat_act, step_size, log_decay, carry_state):
    length = inner_act.shape[0]
    number_blocks = length // STATE_BLOCK

    def split_blocks(values):
        return values.reshape((number_blocks, STATE_BLOCK) + values.shape[1:])
    causal = jnp.arange(STATE_BLOCK)[:, None] >= jnp.arange(STATE_BLOCK)[None, :]

    def advance(running, block_data):
        inner_rows, bmat_rows, cmat_rows, step_rows, decay_rows = block_data
        cumulative = jnp.cumsum(decay_rows, axis=0)
        scores = jnp.einsum('lgn,sgn->lsg', cmat_rows.astype(jnp.float32), bmat_rows.astype(jnp.float32))
        spread = jnp.where(causal[:, :, None, None], cumulative[:, None] - cumulative[None, :], -jnp.inf)
        weights = (scores[:, :, :, None] * jnp.exp(spread) * step_rows[None]).astype(jnp.bfloat16)
        within = jnp.einsum('lsgr,sgrp->lgrp', weights.astype(jnp.float32), inner_rows.astype(jnp.float32))
        carried = jnp.einsum('lgn,grpn->lgrp', cmat_rows.astype(jnp.float32), running, precision=lax.Precision.HIGHEST) * jnp.exp(cumulative)[..., None]
        fading = jnp.exp(cumulative[-1:] - cumulative)
        loaded = (inner_rows.astype(jnp.float32) * (step_rows * fading)[..., None]).astype(jnp.bfloat16)
        running = jnp.exp(cumulative[-1])[..., None, None] * running + jnp.einsum('sgrp,sgn->grpn', loaded.astype(jnp.float32), bmat_rows.astype(jnp.float32))
        return (running, within + carried)
    final_state, outputs = lax.scan(advance, carry_state, tuple((split_blocks(values) for values in (inner_act, bmat_act, cmat_act, step_size, log_decay))))
    return (final_state, outputs.reshape((length,) + outputs.shape[2:]))

def reverse_rows(values):
    return values[::-1]

def reference(inputs, mix_gain, w_query, w_key, w_value, query_gain, key_gain, sink_logit, w_inner, w_bmat, w_cmat, w_gate, w_step, conv_inner, conv_bmat, conv_cmat, step_bias, decay_rate, decay_offset, start_state, group_gain, w_out_attn, w_out_state):
    length = inputs.shape[0]
    widened = inputs.astype(jnp.float32)
    row_scale = lax.rsqrt(lax.optimization_barrier(jnp.mean(widened * widened, axis=1, keepdims=True)) + epsilon)
    scaled_in = (widened * mix_gain).astype(jnp.bfloat16)

    def project(weight):
        return row_scale * jnp.dot(scaled_in, weight, preferred_element_type=jnp.float32)
    query_proj = project(w_query).astype(jnp.bfloat16)
    key_proj = project(w_key).astype(jnp.bfloat16)
    value_proj = project(w_value).astype(jnp.bfloat16)
    inner_proj = project(w_inner).astype(jnp.bfloat16)
    bmat_proj = project(w_bmat).astype(jnp.bfloat16)
    cmat_proj = project(w_cmat).astype(jnp.bfloat16)
    gate_proj = project(w_gate).astype(jnp.bfloat16)
    step_raw = project(w_step.reshape(D, 2 * MIXER_HEADS)).reshape(length, 2, MIXER_HEADS)
    positions = jnp.arange(length, dtype=jnp.int32)
    group_size = A_HEADS // A_KV
    query_rot = rotate(head_norm(query_proj.astype(jnp.float32).reshape(length, A_HEADS, HEAD), query_gain), positions).astype(jnp.bfloat16).reshape(length, A_KV, group_size, HEAD)
    key_rot = rotate(head_norm(key_proj.astype(jnp.float32).reshape(length, A_KV, HEAD), key_gain), positions).astype(jnp.bfloat16)
    value_rows = value_proj.reshape(length, A_KV, HEAD)
    padding = ((WINDOW, WINDOW), (0, 0), (0, 0))
    key_padded = jnp.pad(key_rot, padding)
    value_padded = jnp.pad(value_rows, padding)
    sink_table = sink_logit.reshape(A_KV, group_size)

    def one_block(block_index):
        block_start = (block_index * WINDOW).astype(jnp.int32)
        query_block = lax.dynamic_slice_in_dim(query_rot, block_start, WINDOW, 0)
        key_block = lax.dynamic_slice_in_dim(key_padded, block_start, 3 * WINDOW, 0)
        value_block = lax.dynamic_slice_in_dim(value_padded, block_start, 3 * WINDOW, 0)
        key_pos = block_start - WINDOW + jnp.arange(3 * WINDOW, dtype=jnp.int32)
        return attend_block(query_block, key_block, value_block, sink_table, key_pos, length)
    attended = lax.map(one_block, jnp.arange(length // WINDOW, dtype=jnp.int32))
    attention_out = attended.reshape(length, A_HEADS * HEAD)
    mixed_rows = jnp.concatenate([inner_proj, bmat_proj, cmat_proj], axis=1)
    conv_taps = jnp.concatenate([conv_inner, conv_bmat, conv_cmat], axis=1).astype(jnp.float32)
    rim_width = CONV // 2
    framed = jnp.pad(mixed_rows, ((rim_width, rim_width), (0, 0))).astype(jnp.float32)
    conv_sum = jnp.zeros(mixed_rows.shape, jnp.float32)
    for tap_index in range(CONV):
        conv_sum = conv_sum + framed[tap_index:tap_index + length] * conv_taps[tap_index]
    activated = jax.nn.silu(conv_sum).astype(jnp.bfloat16)
    repeats = MIXER_HEADS // S_GROUPS
    state_width = S_GROUPS * STATE
    inner_act = activated[:, :S_INNER].reshape(length, S_GROUPS, repeats, HEAD)
    bmat_act = activated[:, S_INNER:S_INNER + state_width].reshape(length, S_GROUPS, STATE)
    cmat_act = activated[:, S_INNER + state_width:].reshape(length, S_GROUPS, STATE)
    step_size = jax.nn.softplus(step_raw + step_bias)
    log_decay = -decay_rate * step_size + decay_offset

    def shaped(values):
        return values.reshape(length, S_GROUPS, repeats)
    begin_fwd = start_state[0].reshape(S_GROUPS, repeats, HEAD, STATE)
    begin_bwd = start_state[1].reshape(S_GROUPS, repeats, HEAD, STATE)
    unused_fwd, output_fwd = ssd_blocks(inner_act, bmat_act, cmat_act, shaped(step_size[:, 0]), shaped(log_decay[:, 0]), begin_fwd)
    unused_bwd, output_bwd = ssd_blocks(reverse_rows(inner_act), reverse_rows(bmat_act), reverse_rows(cmat_act), reverse_rows(shaped(step_size[:, 1])), reverse_rows(shaped(log_decay[:, 1])), begin_bwd)
    state_sum = output_fwd + reverse_rows(output_bwd)
    group_width = repeats * HEAD
    gate_rows = gate_proj.astype(jnp.float32).reshape(length, S_GROUPS, group_width)
    gated = state_sum.reshape(length, S_GROUPS, group_width) * jax.nn.silu(gate_rows)
    normed = gated * lax.rsqrt(lax.optimization_barrier(jnp.mean(gated * gated, axis=-1, keepdims=True)) + epsilon)
    state_out = (normed * group_gain.reshape(S_GROUPS, group_width)).astype(jnp.bfloat16).reshape(length, S_INNER)
    attn_cols = A_HEADS * HEAD // N_TP
    state_cols = S_INNER // N_TP
    summed = jnp.zeros((length, D), jnp.float32)
    for part_index in range(N_TP):
        partial_value = jnp.dot(attention_out[:, part_index * attn_cols:(part_index + 1) * attn_cols], w_out_attn[part_index * attn_cols:(part_index + 1) * attn_cols], preferred_element_type=jnp.float32)
        partial_value = partial_value + jnp.dot(state_out[:, part_index * state_cols:(part_index + 1) * state_cols], w_out_state[part_index * state_cols:(part_index + 1) * state_cols], preferred_element_type=jnp.float32)
        summed = summed + lax.optimization_barrier(partial_value.astype(jnp.bfloat16)).astype(jnp.float32)
    return summed.astype(jnp.bfloat16)
```

```python
import functools

import jax
import jax.numpy as jnp
import numpy as np
from jax import lax
from jax.experimental import pallas as pl
from jax.experimental.pallas import tpu as pltpu
from jax.sharding import PartitionSpec as P

HEAD = 64
STATE = 128
CONV = 5
BLK = 128
LANE = 128
ROWS = 256
EDGE = 8

epsilon = 1e-06
rotary_base = 10000.0
F32 = jnp.float32
BF16 = jnp.bfloat16
MESH = pl.DeviceIdType.MESH


def mm(a, b):
    return jnp.dot(a, b, preferred_element_type=F32)


def mm_t(a, b):
    return lax.dot_general(a, b, (((1,), (1,)), ((), ())), preferred_element_type=F32)


def mm_hi(a, b):
    return jnp.dot(a, b, preferred_element_type=F32, precision=lax.Precision.HIGHEST)


def low_half(shape):
    return lax.broadcasted_iota(jnp.int32, shape, len(shape) - 1) < HEAD


def silu(v):
    return v / (1.0 + jnp.exp(-v))


def kernel(
    x_hbm, wq, wk, wv, wi, wb, wc, wg, ws, woa, wos,
    mix_gain, qgain, kgain, sink, taps, bias, rate, offs, start, ggain,
    cos_t, sin_t, cos_o, sin_o, expand,
    out_ref,
    w, wo, xown, xpeer, xs, rs, kv, xbuf, qb, gb, st, cb, act, gs, dec, sb, z,
    psend, precv, kvlo, kvhi, xlo, xhi, chain_s, chain_r, sem_w, sem_x, sem_xs, sem_xr,
    sem_hs, sem_hr, sem_cs, sem_cr, sem_ps, sem_pr,
    *, n_sp,
):
    me = lax.axis_index("tp")
    idx = lax.axis_index("sp")
    peer = 1 - me
    T, half = x_hbm.shape
    nb = T // BLK
    nchunk = T // ROWS
    has_prev = idx > 0
    has_next = idx < n_sp - 1

    barrier = pltpu.get_barrier_semaphore()
    pl.semaphore_signal(barrier, inc=1, device_id={"tp": peer}, device_id_type=MESH)

    @pl.when(has_prev)
    def _():
        pl.semaphore_signal(barrier, inc=1, device_id={"sp": idx - 1}, device_id_type=MESH)

    @pl.when(has_next)
    def _():
        pl.semaphore_signal(barrier, inc=1, device_id={"sp": idx + 1}, device_id_type=MESH)

    own_copies = []
    for i in range(nchunk):
        c = pltpu.make_async_copy(
            x_hbm.at[pl.ds(i * ROWS, ROWS)], xown.at[pl.ds(i * ROWS, ROWS)], sem_x.at[i]
        )
        c.start()
        own_copies.append(c)
    wcopies = []
    col = 0
    for j, src in enumerate((wk, wv, wi, wb, wc, wq, wg, ws)):
        width = src.shape[1]
        c = pltpu.make_async_copy(src, w.at[:, pl.ds(col, width)], sem_w.at[j])
        c.start()
        wcopies.append(c)
        col += width
    n_w = len(wcopies)
    na = woa.shape[0]
    oc = [
        pltpu.make_async_copy(woa, wo.at[pl.ds(0, na)], sem_w.at[n_w]),
        pltpu.make_async_copy(wos, wo.at[pl.ds(na, wos.shape[0])], sem_w.at[n_w + 1]),
    ]
    for c in oc:
        c.start()

    @pl.when(has_prev & has_next)
    def _():
        pl.semaphore_wait(barrier, 3)

    @pl.when(jnp.logical_not(has_prev & has_next))
    def _():
        pl.semaphore_wait(barrier, 2 if n_sp > 1 else 1)

    gath = []
    for i in range(nchunk):
        c = pltpu.make_async_remote_copy(
            src_ref=x_hbm.at[pl.ds(i * ROWS, ROWS)],
            dst_ref=xpeer.at[pl.ds(i * ROWS, ROWS)],
            send_sem=sem_xs.at[i],
            recv_sem=sem_xr.at[i],
            device_id={"tp": peer},
            device_id_type=MESH,
        )
        c.start()
        gath.append(c)

    gain_own = mix_gain[:, pl.ds(pl.multiple_of(me * half, LANE), half)]
    gain_peer = mix_gain[:, pl.ds(pl.multiple_of(peer * half, LANE), half)]
    for i in range(nchunk):
        own_copies[i].wait()
        gath[i].wait()

        def scale_rows(r, carry):
            rows = pl.ds(pl.multiple_of(i * ROWS + r * 32, 32), 32)
            a = xown[rows, :].astype(F32)
            b = xpeer[rows, :].astype(F32)
            total = jnp.sum(a * a + b * b, axis=1, keepdims=True)
            rs[rows, :] = jnp.broadcast_to(
                lax.rsqrt(total * (1.0 / (2 * half)) + epsilon), (32, LANE)
            )
            xs[rows, pl.ds(pl.multiple_of(me * half, LANE), half)] = (a * gain_own).astype(BF16)
            xs[rows, pl.ds(pl.multiple_of(peer * half, LANE), half)] = (b * gain_peer).astype(BF16)
            return carry

        lax.fori_loop(0, ROWS // 32, scale_rows, 0)

    co = cos_o[pl.ds(idx, 1), :]
    so = sin_o[pl.ds(idx, 1), :]

    def norm_rotate(v, gain, rows):
        shape = v.shape
        low = low_half(shape)
        sq = v * v
        s_lo = jnp.sum(jnp.where(low, sq, 0.0), axis=1, keepdims=True)
        s_hi = jnp.sum(jnp.where(low, 0.0, sq), axis=1, keepdims=True)
        v = v * lax.rsqrt(jnp.where(low, s_lo, s_hi) * (1.0 / HEAD) + epsilon) * gain
        ct = cos_t[rows, :]
        sn = sin_t[rows, :]
        cosine = co * ct - so * sn
        sine = so * ct + co * sn
        first = (lax.broadcasted_iota(jnp.int32, shape, 1) % HEAD) < HEAD // 2
        partner = jnp.where(first, -pltpu.roll(v, LANE - HEAD // 2, 1), pltpu.roll(v, HEAD // 2, 1))
        return v * cosine + partner * sine

    def row_chunk(i):
        start_row = pl.multiple_of(i * ROWS, ROWS)
        return start_row, pl.ds(start_row, ROWS)

    kvw = wk.shape[1]
    wcopies[0].wait()
    wcopies[1].wait()

    def kv_step(i, carry):
        r0, rows = row_chunk(i)
        p = mm(xs[rows, :], w[:, : 2 * kvw])
        scale = rs[rows, :]
        k = (p[:, :LANE] * scale).astype(BF16).astype(F32)
        v = (p[:, LANE:] * scale).astype(BF16).astype(F32)
        k = norm_rotate(k, kgain[...], rows)
        low = low_half(k.shape)
        k_sw = pltpu.roll(k, HEAD, 1)
        v_sw = pltpu.roll(v, HEAD, 1)
        dst = pl.ds(pl.multiple_of(r0 + BLK, BLK), ROWS)
        kv[dst, 0:LANE] = jnp.where(low, k, k_sw).astype(BF16)
        kv[dst, LANE : 2 * LANE] = jnp.where(low, k_sw, k).astype(BF16)
        kv[dst, 2 * LANE : 3 * LANE] = jnp.where(low, v, v_sw).astype(BF16)
        kv[dst, 3 * LANE : 4 * LANE] = jnp.where(low, v_sw, v).astype(BF16)
        return carry

    lax.fori_loop(0, nchunk, kv_step, 0)

    def remote(src, dst, ss, rsem, target):
        return pltpu.make_async_remote_copy(
            src_ref=src, dst_ref=dst, send_sem=ss, recv_sem=rsem,
            device_id={"sp": target}, device_id_type=MESH,
        )

    inner_w = wi.shape[1]
    state_w = wb.shape[1]
    xw = inner_w + 2 * state_w
    for j in (2, 3, 4):
        wcopies[j].wait()

    def x_step(i, carry):
        r0, rows = row_chunk(i)
        scale = rs[rows, :]
        dst = pl.ds(pl.multiple_of(r0 + EDGE, EDGE), ROWS)
        for s in range(0, xw, 256):
            p = mm(xs[rows, :], w[:, 2 * kvw + s : 2 * kvw + s + 256])
            for t in range(0, 256, LANE):
                xbuf[dst, s + t : s + t + LANE] = (p[:, t : t + LANE] * scale).astype(BF16).astype(F32)
        return carry

    kv_up = remote(kv.at[pl.ds(T, BLK)], kvlo, sem_hs.at[0], sem_hr.at[0], idx + 1)
    kv_dn = remote(kv.at[pl.ds(BLK, BLK)], kvhi, sem_hs.at[1], sem_hr.at[1], idx - 1)
    x_up = remote(xbuf.at[pl.ds(T, EDGE)], xlo, sem_hs.at[2], sem_hr.at[2], idx + 1)
    x_dn = remote(xbuf.at[pl.ds(EDGE, EDGE)], xhi, sem_hs.at[3], sem_hr.at[3], idx - 1)

    x_step(0, 0)

    @pl.when(has_next)
    def _():
        kv_up.start()

    @pl.when(has_prev)
    def _():
        kv_dn.start()

    lax.fori_loop(1, nchunk, x_step, 0)

    for j in (5, 6, 7):
        wcopies[j].wait()
    qcol = 2 * kvw + xw
    qw = wq.shape[1]
    gw = wg.shape[1]

    def q_step(i, carry):
        r0, rows = row_chunk(i)
        scale = rs[rows, :]
        xr = xs[rows, :]
        for s in range(0, qw, 256):
            p = mm(xr, w[:, qcol + s : qcol + s + 256])
            for t in range(0, 256, LANE):
                q = (p[:, t : t + LANE] * scale).astype(BF16).astype(F32)
                q = norm_rotate(q, qgain[...], rows).astype(BF16).astype(F32)
                qb[rows, s + t : s + t + LANE] = (q * HEAD ** (-0.5)).astype(BF16)
        for s in range(0, gw, 256):
            p = mm(xr, w[:, qcol + qw + s : qcol + qw + s + 256])
            for t in range(0, 256, LANE):
                gb[rows, s + t : s + t + LANE] = (p[:, t : t + LANE] * scale).astype(BF16)
        p = mm(xr, w[:, qcol + qw + gw :]) * scale + bias[...]
        step = jnp.maximum(p, 0.0) + jnp.log1p(jnp.exp(-jnp.abs(p)))
        st[rows, :] = step
        cb[rows, :] = -rate[...] * step + offs[rows, :]
        return carry

    q_step(0, 0)

    @pl.when(has_next)
    def _():
        x_up.start()

    @pl.when(has_prev)
    def _():
        x_dn.start()

    lax.fori_loop(1, nchunk, q_step, 0)

    @pl.when(has_next)
    def _():
        kv_up.wait_send()
        x_up.wait_send()
        kv_dn.wait_recv()
        x_dn.wait_recv()
        kv[pl.ds(T + BLK, BLK), :] = kvhi[...]
        xbuf[pl.ds(T + EDGE, EDGE), :] = xhi[...]

    @pl.when(jnp.logical_not(has_next))
    def _():
        kv[pl.ds(T + BLK, BLK), :] = jnp.zeros((BLK, kv.shape[1]), BF16)
        xbuf[pl.ds(T + EDGE, EDGE), :] = jnp.zeros((EDGE, xw), F32)

    @pl.when(has_prev)
    def _():
        kv_dn.wait_send()
        x_dn.wait_send()
        kv_up.wait_recv()
        x_up.wait_recv()
        kv[pl.ds(0, BLK), :] = kvlo[...]
        xbuf[pl.ds(0, EDGE), :] = xlo[...]

    @pl.when(jnp.logical_not(has_prev))
    def _():
        kv[pl.ds(0, BLK), :] = jnp.zeros((BLK, kv.shape[1]), BF16)
        xbuf[pl.ds(0, EDGE), :] = jnp.zeros((EDGE, xw), F32)

    sq = (BLK, BLK)
    ri = lax.broadcasted_iota(jnp.int32, sq, 0)
    ci = lax.broadcasted_iota(jnp.int32, sq, 1)
    heads = inner_w // HEAD
    groups = state_w // STATE
    per_group = heads // groups
    gwid = per_group * HEAD
    low = low_half(sq)

    def spread(values, column):
        return jnp.broadcast_to(values[:, column : column + 1], sq)

    def paired(values, tile, direction):
        base = direction * heads + 2 * tile
        return jnp.where(low, spread(values, base), spread(values, base + 1))

    def state_step(b, carry):
        rows = pl.ds(pl.multiple_of(b * BLK, BLK), BLK)
        lower = jnp.where(ri >= ci, 1.0, 0.0).astype(F32)
        upper = jnp.where(ri <= ci, 1.0, 0.0).astype(F32)
        d = cb[rows, :]
        c = jnp.where(ci < heads, mm_hi(lower, d), mm_hi(upper, d))
        cb[rows, :] = c
        last = jnp.where(ci[:1] < heads, c[BLK - 1 : BLK, :], c[0:1, :])
        last8 = jnp.broadcast_to(last, (8, BLK))
        wide = jnp.exp(mm_hi(last8, expand[...]))
        dec[b, 0] = wide[:, :inner_w]
        dec[b, 1] = wide[:, inner_w:]
        load = st[rows, :] * jnp.exp(last - c)
        bt = []
        for s in range(xw - LANE, -1, -LANE):
            win = xbuf[pl.ds(pl.multiple_of(b * BLK, BLK), BLK + 2 * EDGE), s : s + LANE]
            acc = jnp.zeros(sq, F32)
            for j in range(CONV):
                o = EDGE - CONV // 2 + j
                acc = acc + win[o : o + BLK] * taps[j : j + 1, s : s + LANE]
            a = silu(acc).astype(BF16)
            act[rows, s : s + LANE] = a
            if inner_w <= s < inner_w + state_w:
                bt.insert(0, a.astype(F32).T.astype(BF16))
            if s < inner_w:
                tile = s // LANE
                g = s // gwid
                af = a.astype(F32)
                for direction in range(2):
                    loaded = (af * paired(load, tile, direction)).astype(BF16)
                    gs[b, direction, :, s : s + LANE] = mm(bt[g], loaded)
        return carry

    lax.fori_loop(0, nb, state_step, 0)

    up = remote(chain_s.at[0], chain_r.at[0], sem_cs.at[0], sem_cr.at[0], idx + 1)
    dn = remote(chain_s.at[1], chain_r.at[1], sem_cs.at[1], sem_cr.at[1], idx - 1)

    def hop(direction, copy, first, has_source, has_target):
        @pl.when(has_source)
        def _():
            copy.wait_recv()

        @pl.when(has_target)
        def _():
            order = list(range(nb)) if direction == 0 else list(range(nb - 1, -1, -1))
            for s in range(0, inner_w, LANE):
                cols = slice(s, s + LANE)
                enter = jnp.where(
                    has_source, chain_r[direction, :, cols].astype(F32), start[direction, :, cols]
                )
                total = enter
                for b in order:
                    total = total * dec[b, direction, 0:1, cols] + gs[b, direction, :, cols]
                chain_s[direction, :, cols] = total.astype(BF16)

    key_w = 3 * BLK
    aj = lax.broadcasted_iota(jnp.int32, (BLK, key_w), 1)
    ai = lax.broadcasted_iota(jnp.int32, (BLK, key_w), 0)
    reach = 2 * BLK
    kv_heads = kvw // HEAD
    q_per = (qw // HEAD) // kv_heads
    ones = jnp.ones((key_w, LANE), BF16)
    turn_up = (idx * nb) // n_sp
    turn_dn = ((n_sp - 1 - idx) * nb) // n_sp

    def attend(b, carry):
        @pl.when(b == turn_up)
        def _():
            hop(0, up, idx == 0, has_prev, has_next)

        @pl.when(b == turn_dn)
        def _():
            hop(1, dn, idx == n_sp - 1, has_next, has_prev)

        rows = pl.ds(pl.multiple_of(b * BLK, BLK), BLK)
        span = pl.ds(pl.multiple_of(b * BLK, BLK), key_w)
        lo = jnp.where((idx == 0) & (b == 0), BLK, 0)
        hi = jnp.where((idx == n_sp - 1) & (b == nb - 1), 2 * BLK - 1, key_w)
        valid = (aj >= jnp.maximum(ai, lo)) & (aj <= jnp.minimum(ai + reach, hi))
        for g in range(kv_heads):
            parts = []
            for t in range(q_per // 2):
                tile = g * (q_per // 2) + t
                q = qb[rows, tile * LANE : (tile + 1) * LANE]
                zero = jnp.zeros_like(q)
                parts += [jnp.where(low, q, zero), jnp.where(low, zero, q)]
            keys = kv[span, g * LANE : (g + 1) * LANE]
            vals = kv[span, (kv_heads + g) * LANE : (kv_heads + g + 1) * LANE]
            ext = jnp.concatenate([vals, ones], axis=1)
            s_all = mm_t(jnp.concatenate(parts, axis=0), keys)
            outs = []
            for r in range(q_per):
                s = jnp.where(valid, s_all[r * BLK : (r + 1) * BLK], -1e30)
                sk = sink[g * q_per + r : g * q_per + r + 1, :]
                m = jnp.maximum(jnp.max(s, axis=1, keepdims=True), sk[:, :1])
                p = jnp.where(valid, jnp.exp(s - m), 0.0).astype(BF16)
                o = mm(p, ext)
                den = o[:, LANE:] + jnp.exp(sk - m)
                outs.append(o[:, :LANE] / den)
            for t in range(q_per // 2):
                tile = g * (q_per // 2) + t
                z[rows, tile * LANE : (tile + 1) * LANE] = jnp.where(
                    low, outs[2 * t], outs[2 * t + 1]
                ).astype(BF16)

        @pl.when((b == turn_up) & has_next)
        def _():
            up.start()

        @pl.when((b == turn_dn) & has_prev)
        def _():
            dn.start()

        return carry

    lax.fori_loop(0, nb, attend, 0)

    @pl.when(has_next)
    def _():
        up.wait_send()

    @pl.when(has_prev)
    def _():
        dn.wait_send()

    for direction in range(2):
        source = has_prev if direction == 0 else has_next
        order = list(range(nb)) if direction == 0 else list(range(nb - 1, -1, -1))
        for s in range(0, inner_w, LANE):
            cols = slice(s, s + LANE)
            total = jnp.where(
                source, chain_r[direction, :, cols].astype(F32), start[direction, :, cols]
            )
            for b in order:
                sb[b, direction, :, cols] = total.astype(BF16)
                if b != order[-1]:
                    total = total * dec[b, direction, 0:1, cols] + gs[b, direction, :, cols]

    attn_w = qw

    def mix_block(b):
        rows = pl.ds(pl.multiple_of(b * BLK, BLK), BLK)
        c = cb[rows, :]
        step = st[rows, :]
        c_t = c.T
        step_t = step.T
        diag = ri == ci
        below = ri >= ci
        for g in range(groups):
            bm = act[rows, inner_w + g * STATE : inner_w + (g + 1) * STATE]
            cm = act[rows, inner_w + state_w + g * STATE : inner_w + state_w + (g + 1) * STATE]
            scores = mm_t(cm, bm)
            carried = [mm(cm, sb[b, d, :, g * gwid : (g + 1) * gwid]) for d in range(2)]
            gated = []
            for t in range(per_group // 2):
                tile = g * (per_group // 2) + t
                ws_ = []
                cols_f, cols_b = [], []
                for u in range(2):
                    h = 2 * tile + u
                    cf = spread(c, h)
                    cr = spread(c, heads + h)
                    cols_f.append(cf)
                    cols_b.append(cr)
                    arg = jnp.where(
                        below, cf - c_t[h : h + 1, :], cr - c_t[heads + h : heads + h + 1, :]
                    )
                    sf = step_t[h : h + 1, :]
                    sr = step_t[heads + h : heads + h + 1, :]
                    fac = jnp.where(diag, sf + sr, jnp.where(below, sf, sr))
                    ws_.append((scores * jnp.exp(arg) * fac).astype(BF16))
                y = mm(jnp.concatenate(ws_, axis=0), act[rows, tile * LANE : (tile + 1) * LANE])
                y = jnp.where(low, y[:BLK], y[BLK:])
                seg = slice(t * LANE, (t + 1) * LANE)
                y = y + carried[0][:, seg] * jnp.exp(jnp.where(low, cols_f[0], cols_f[1]))
                y = y + carried[1][:, seg] * jnp.exp(jnp.where(low, cols_b[0], cols_b[1]))
                gated.append(y * silu(gb[rows, tile * LANE : (tile + 1) * LANE].astype(F32)))
            total = sum(jnp.sum(v * v, axis=1, keepdims=True) for v in gated)
            inv = lax.rsqrt(total * (1.0 / gwid) + epsilon)
            for t, v in enumerate(gated):
                s = g * gwid + t * LANE
                z[rows, attn_w + s : attn_w + s + LANE] = (
                    v * inv * ggain[:, s : s + LANE]
                ).astype(BF16)

    for c in oc:
        c.wait()
    half_rows = T // 2
    steps = half_rows // ROWS
    width = wo.shape[1]

    def mix_rows(base):
        def one(k, carry):
            mix_block(base // BLK + k)
            return carry

        lax.fori_loop(0, ROWS // BLK, one, 0)

    copies = []
    for i in range(steps):
        base = peer * half_rows + i * ROWS
        mix_rows(base)
        zr = z[pl.ds(pl.multiple_of(base, ROWS), ROWS), :]
        for s in range(0, width, 512):
            psend[i * ROWS : (i + 1) * ROWS, s : s + 512] = mm(zr, wo[:, s : s + 512]).astype(BF16)
        copies.append(
            pltpu.make_async_remote_copy(
                src_ref=psend.at[pl.ds(i * ROWS, ROWS)],
                dst_ref=precv.at[pl.ds(i * ROWS, ROWS)],
                send_sem=sem_ps.at[i],
                recv_sem=sem_pr.at[i],
                device_id={"tp": peer},
                device_id_type=MESH,
            )
        )
        if i > 0:
            copies[i - 1].start()
    for i in range(steps):
        base = me * half_rows + i * ROWS
        mix_rows(base)
        if i == 0:
            copies[-1].start()
        zr = z[pl.ds(pl.multiple_of(base, ROWS), ROWS), :]
        for s in range(0, width, 512):
            part = mm(zr, wo[:, s : s + 512]).astype(BF16).astype(F32)
            if s == 0:
                copies[i].wait()
            got = precv[i * ROWS : (i + 1) * ROWS, s : s + 512].astype(F32)
            out_ref[i * ROWS : (i + 1) * ROWS, s : s + 512] = (part + got).astype(BF16)


def tables(tokens, count):
    lane = np.arange(LANE) % (HEAD // 2)
    frequency = rotary_base ** (-lane.astype(np.float64) / (HEAD // 2))
    inner = np.arange(tokens, dtype=np.float64)[:, None] * frequency[None, :]
    outer = np.arange(count, dtype=np.float64)[:, None] * tokens * frequency[None, :]
    return [f(a).astype(np.float32) for a in (inner, outer) for f in (np.cos, np.sin)]


def local(
    n_sp,
    inputs, mix_gain, w_query, w_key, w_value, query_gain, key_gain, sink_logit,
    w_inner, w_bmat, w_cmat, w_gate, w_step, conv_inner, conv_bmat, conv_cmat,
    step_bias, decay_rate, decay_offset, start_state, group_gain, w_out_attn, w_out_state,
):
    T, half = inputs.shape
    depth = w_query.shape[0]
    heads = w_step.shape[2]
    inner_w = w_inner.shape[1]
    state_w = w_bmat.shape[1]
    xw = inner_w + 2 * state_w
    kvw = w_key.shape[1]
    qw = w_query.shape[1]
    gw = w_gate.shape[1]
    width = w_out_attn.shape[1]
    nb = T // BLK
    nchunk = T // ROWS

    def lanes(a):
        return jnp.pad(a, ((0, 0), (0, LANE - a.shape[1])))

    ws = lanes(w_step.reshape(depth, -1))
    bias = lanes(step_bias.reshape(1, -1))
    rate = lanes(decay_rate.reshape(1, -1))
    offs = lanes(decay_offset.reshape(T, -1))
    taps = jnp.concatenate([conv_inner, conv_bmat, conv_cmat], axis=1).astype(F32)
    start = start_state.reshape(2, inner_w, STATE).transpose(0, 2, 1)
    sink = jnp.broadcast_to(sink_logit[:, None], (sink_logit.shape[0], LANE))
    twice = LANE // HEAD
    ct, sn, co, so = tables(T, n_sp)
    expand = np.zeros((LANE, 2 * inner_w), np.float32)
    for c in range(2 * heads):
        expand[c, c * HEAD : (c + 1) * HEAD] = 1.0
    any_spec = pl.BlockSpec(memory_space=pl.ANY)
    vm = pl.BlockSpec(memory_space=pltpu.VMEM)
    wcols = 2 * kvw + xw + qw + gw + LANE
    V = pltpu.VMEM
    dma = pltpu.SemaphoreType.DMA
    steps = T // 2 // ROWS
    scratch = [
        V((depth, wcols), BF16),
        V((w_out_attn.shape[0] + w_out_state.shape[0], width), BF16),
        V((T, half), BF16), V((T, half), BF16), V((T, 2 * half), BF16), V((T, LANE), F32),
        V((T + 2 * BLK, 4 * LANE), BF16), V((T + 2 * EDGE, xw), F32),
        V((T, qw), BF16), V((T, gw), BF16), V((T, LANE), F32), V((T, LANE), F32),
        V((T, xw), BF16),
        V((nb, 2, STATE, inner_w), F32), V((nb, 2, 8, inner_w), F32),
        V((nb, 2, STATE, inner_w), BF16),
        V((T, qw + inner_w), BF16),
        V((T // 2, width), BF16), V((T // 2, width), BF16),
        V((BLK, 4 * LANE), BF16), V((BLK, 4 * LANE), BF16),
        V((EDGE, xw), F32), V((EDGE, xw), F32),
        V((2, STATE, inner_w), BF16), V((2, STATE, inner_w), BF16),
        dma((10,)), dma((nchunk,)), dma((nchunk,)), dma((nchunk,)),
        dma((4,)), dma((4,)), dma((2,)), dma((2,)), dma((steps,)), dma((steps,)),
    ]
    return pl.pallas_call(
        functools.partial(kernel, n_sp=n_sp),
        out_shape=jax.ShapeDtypeStruct((T // 2, width), BF16),
        in_specs=[any_spec] * 11 + [vm] * 15,
        out_specs=vm,
        scratch_shapes=scratch,
        compiler_params=pltpu.CompilerParams(
            collective_id=0, has_side_effects=True, vmem_limit_bytes=67043328
        ),
        name="mixer",
    )(
        inputs, w_query, w_key, w_value, w_inner, w_bmat, w_cmat, w_gate, ws,
        w_out_attn, w_out_state,
        mix_gain.reshape(1, -1), jnp.tile(query_gain, twice).reshape(1, -1),
        jnp.tile(key_gain, twice).reshape(1, -1), sink, taps, bias, rate, offs, start,
        group_gain.reshape(1, -1), jnp.asarray(ct), jnp.asarray(sn), jnp.asarray(co),
        jnp.asarray(so), jnp.asarray(expand),
    )


def solution(mesh):
    return jax.shard_map(
        functools.partial(local, mesh.shape["sp"]),
        mesh=mesh,
        in_specs=(
            P(("fs", "sp"), "tp"),
            P(),
            P(None, "tp"),
            P(None, "tp"),
            P(None, "tp"),
            P(),
            P(),
            P("tp"),
            P(None, "tp"),
            P(None, "tp"),
            P(None, "tp"),
            P(None, "tp"),
            P(None, None, "tp"),
            P(None, "tp"),
            P(None, "tp"),
            P(None, "tp"),
            P(None, "tp"),
            P(None, "tp"),
            P("sp", None, "tp"),
            P("fs", "tp", None, None),
            P("tp"),
            P("tp", None),
            P("tp", None),
        ),
        out_specs=P(("fs", "sp", "tp"), None),
        check_vma=False,
    )
```

```python
import functools

import jax
import jax.numpy as jnp
import numpy as np
from jax import lax
from jax.experimental import pallas as pl
from jax.experimental.pallas import tpu as pltpu
from jax.sharding import PartitionSpec as P

HEAD = 64
STATE = 128
CONV = 5
BLK = 128
LANE = 128
ROWS = 256
EDGE = 8

epsilon = 1e-06
rotary_base = 10000.0
F32 = jnp.float32
BF16 = jnp.bfloat16
MESH = pl.DeviceIdType.MESH


def mm(a, b):
    return jnp.dot(a, b, preferred_element_type=F32)


def mm_t(a, b):
    return lax.dot_general(a, b, (((1,), (1,)), ((), ())), preferred_element_type=F32)


def mm_hi(a, b):
    return jnp.dot(a, b, preferred_element_type=F32, precision=lax.Precision.HIGHEST)


def low_half(shape):
    return lax.broadcasted_iota(jnp.int32, shape, len(shape) - 1) < HEAD


def silu(v):
    return v / (1.0 + jnp.exp(-v))


def kernel(
    x_hbm, wq, wk, wv, wi, wb, wc, wg, ws, woa, wos,
    mix_gain, qgain1, kgain1, sink, taps_i, taps_b, taps_c, bias2, rate2, offs, start, ggain,
    cos_t, sin_t, cos_o, sin_o, expand,
    out_ref,
    w, wst, wo, xown, xpeer, xs, rs, kv, xbuf, qb, gb, st, cb, act, gs, dec, sb, z,
    psend, precv, kvlo, kvhi, xlo, xhi, chain_s, chain_r, sem_w, sem_x, sem_xs, sem_xr,
    sem_hs, sem_hr, sem_cs, sem_cr, sem_ps, sem_pr,
    *, n_sp,
):
    me = lax.axis_index("tp")
    idx = lax.axis_index("sp")
    peer = 1 - me
    T, half = x_hbm.shape
    nb = T // BLK
    nchunk = T // ROWS
    has_prev = idx > 0
    has_next = idx < n_sp - 1

    barrier = pltpu.get_barrier_semaphore()
    pl.semaphore_signal(barrier, inc=1, device_id={"tp": peer}, device_id_type=MESH)

    @pl.when(has_prev)
    def _():
        pl.semaphore_signal(barrier, inc=1, device_id={"sp": idx - 1}, device_id_type=MESH)

    @pl.when(has_next)
    def _():
        pl.semaphore_signal(barrier, inc=1, device_id={"sp": idx + 1}, device_id_type=MESH)

    own_copies = []
    for i in range(nchunk):
        c = pltpu.make_async_copy(
            x_hbm.at[pl.ds(i * ROWS, ROWS)], xown.at[pl.ds(i * ROWS, ROWS)], sem_x.at[i]
        )
        c.start()
        own_copies.append(c)
    wcopies = []
    col = 0
    for j, src in enumerate((wk, wv, wi, wb, wc, wq, wg, ws)):
        width = src.shape[1]
        dst = w.at[:, pl.ds(col, width)] if src is not ws else wst
        c = pltpu.make_async_copy(src, dst, sem_w.at[j])
        c.start()
        wcopies.append(c)
        col += width
    n_w = len(wcopies)
    na = woa.shape[0]
    oc = [
        pltpu.make_async_copy(woa, wo.at[pl.ds(0, na)], sem_w.at[n_w]),
        pltpu.make_async_copy(wos, wo.at[pl.ds(na, wos.shape[0])], sem_w.at[n_w + 1]),
    ]
    for c in oc:
        c.start()

    st[...] = jnp.zeros_like(st)
    cb[...] = jnp.zeros_like(cb)
    qgain = jnp.concatenate([qgain1[...]] * (LANE // HEAD), axis=1)
    kgain = jnp.concatenate([kgain1[...]] * (LANE // HEAD), axis=1)
    bias = jnp.concatenate([bias2[0:1, :], bias2[1:2, :]], axis=1)
    rate = jnp.concatenate([rate2[0:1, :], rate2[1:2, :]], axis=1)

    @pl.when(has_prev & has_next)
    def _():
        pl.semaphore_wait(barrier, 3)

    @pl.when(jnp.logical_not(has_prev & has_next))
    def _():
        pl.semaphore_wait(barrier, 2 if n_sp > 1 else 1)

    gath = []
    for i in range(nchunk):
        c = pltpu.make_async_remote_copy(
            src_ref=x_hbm.at[pl.ds(i * ROWS, ROWS)],
            dst_ref=xpeer.at[pl.ds(i * ROWS, ROWS)],
            send_sem=sem_xs.at[i],
            recv_sem=sem_xr.at[i],
            device_id={"tp": peer},
            device_id_type=MESH,
        )
        c.start()
        gath.append(c)

    gain_own = mix_gain[:, pl.ds(pl.multiple_of(me * half, LANE), half)]
    gain_peer = mix_gain[:, pl.ds(pl.multiple_of(peer * half, LANE), half)]
    for i in range(nchunk):
        own_copies[i].wait()
        gath[i].wait()

        def scale_rows(r, carry):
            rows = pl.ds(pl.multiple_of(i * ROWS + r * 32, 32), 32)
            a = xown[rows, :].astype(F32)
            b = xpeer[rows, :].astype(F32)
            total = jnp.sum(a * a + b * b, axis=1, keepdims=True)
            rs[rows, :] = jnp.broadcast_to(
                lax.rsqrt(total * (1.0 / (2 * half)) + epsilon), (32, LANE)
            )
            xs[rows, pl.ds(pl.multiple_of(me * half, LANE), half)] = (a * gain_own).astype(BF16)
            xs[rows, pl.ds(pl.multiple_of(peer * half, LANE), half)] = (b * gain_peer).astype(BF16)
            return carry

        lax.fori_loop(0, ROWS // 32, scale_rows, 0)

    co = cos_o[pl.ds(idx, 1), :]
    so = sin_o[pl.ds(idx, 1), :]

    def norm_rotate(v, gain, rows):
        shape = v.shape
        low = low_half(shape)
        sq = v * v
        s_lo = jnp.sum(jnp.where(low, sq, 0.0), axis=1, keepdims=True)
        s_hi = jnp.sum(jnp.where(low, 0.0, sq), axis=1, keepdims=True)
        v = v * lax.rsqrt(jnp.where(low, s_lo, s_hi) * (1.0 / HEAD) + epsilon) * gain
        ct = cos_t[rows, :]
        sn = sin_t[rows, :]
        cosine = co * ct - so * sn
        sine = so * ct + co * sn
        first = (lax.broadcasted_iota(jnp.int32, shape, 1) % HEAD) < HEAD // 2
        partner = jnp.where(first, -pltpu.roll(v, LANE - HEAD // 2, 1), pltpu.roll(v, HEAD // 2, 1))
        return v * cosine + partner * sine

    def row_chunk(i):
        start_row = pl.multiple_of(i * ROWS, ROWS)
        return start_row, pl.ds(start_row, ROWS)

    kvw = wk.shape[1]
    wcopies[0].wait()
    wcopies[1].wait()

    def kv_step(i, carry):
        r0, rows = row_chunk(i)
        p = mm(xs[rows, :], w[:, : 2 * kvw])
        scale = rs[rows, :]
        k = (p[:, :LANE] * scale).astype(BF16).astype(F32)
        v = (p[:, LANE:] * scale).astype(BF16).astype(F32)
        k = norm_rotate(k, kgain, rows)
        low = low_half(k.shape)
        k_sw = pltpu.roll(k, HEAD, 1)
        v_sw = pltpu.roll(v, HEAD, 1)
        dst = pl.ds(pl.multiple_of(r0 + BLK, BLK), ROWS)
        kv[dst, 0:LANE] = jnp.where(low, k, k_sw).astype(BF16)
        kv[dst, LANE : 2 * LANE] = jnp.where(low, k_sw, k).astype(BF16)
        kv[dst, 2 * LANE : 3 * LANE] = jnp.where(low, v, v_sw).astype(BF16)
        kv[dst, 3 * LANE : 4 * LANE] = jnp.where(low, v_sw, v).astype(BF16)
        return carry

    lax.fori_loop(0, nchunk, kv_step, 0)

    def remote(src, dst, ss, rsem, target):
        return pltpu.make_async_remote_copy(
            src_ref=src, dst_ref=dst, send_sem=ss, recv_sem=rsem,
            device_id={"sp": target}, device_id_type=MESH,
        )

    inner_w = wi.shape[1]
    state_w = wb.shape[1]
    xw = inner_w + 2 * state_w
    for j in (2, 3, 4):
        wcopies[j].wait()

    def x_step(i, carry):
        r0, rows = row_chunk(i)
        scale = rs[rows, :]
        dst = pl.ds(pl.multiple_of(r0 + EDGE, EDGE), ROWS)
        for s in range(0, xw, 256):
            p = mm(xs[rows, :], w[:, 2 * kvw + s : 2 * kvw + s + 256])
            for t in range(0, 256, LANE):
                xbuf[dst, s + t : s + t + LANE] = (p[:, t : t + LANE] * scale).astype(BF16).astype(F32)
        return carry

    kv_up = remote(kv.at[pl.ds(T, BLK)], kvlo, sem_hs.at[0], sem_hr.at[0], idx + 1)
    kv_dn = remote(kv.at[pl.ds(BLK, BLK)], kvhi, sem_hs.at[1], sem_hr.at[1], idx - 1)
    x_up = remote(xbuf.at[pl.ds(T, EDGE)], xlo, sem_hs.at[2], sem_hr.at[2], idx + 1)
    x_dn = remote(xbuf.at[pl.ds(EDGE, EDGE)], xhi, sem_hs.at[3], sem_hr.at[3], idx - 1)

    x_step(0, 0)

    @pl.when(has_next)
    def _():
        kv_up.start()

    @pl.when(has_prev)
    def _():
        kv_dn.start()

    lax.fori_loop(1, nchunk, x_step, 0)

    for j in (5, 6, 7):
        wcopies[j].wait()
    qcol = 2 * kvw + xw
    qw = wq.shape[1]
    gw = wg.shape[1]

    def q_step(i, carry):
        r0, rows = row_chunk(i)
        scale = rs[rows, :]
        xr = xs[rows, :]
        for s in range(0, qw, 256):
            p = mm(xr, w[:, qcol + s : qcol + s + 256])
            for t in range(0, 256, LANE):
                q = (p[:, t : t + LANE] * scale).astype(BF16).astype(F32)
                q = norm_rotate(q, qgain, rows).astype(BF16).astype(F32)
                qb[rows, s + t : s + t + LANE] = (q * HEAD ** (-0.5)).astype(BF16)
        for s in range(0, gw, 256):
            p = mm(xr, w[:, qcol + qw + s : qcol + qw + s + 256])
            for t in range(0, 256, LANE):
                gb[rows, s + t : s + t + LANE] = (p[:, t : t + LANE] * scale).astype(BF16)
        p = mm(xr, wst[...]) * scale[:, : wst.shape[1]] + bias
        step = jnp.maximum(p, 0.0) + jnp.log1p(jnp.exp(-jnp.abs(p)))
        st[rows, : wst.shape[1]] = step
        cb[rows, : wst.shape[1]] = -rate * step + offs[rows, :]
        return carry

    q_step(0, 0)

    @pl.when(has_next)
    def _():
        x_up.start()

    @pl.when(has_prev)
    def _():
        x_dn.start()

    lax.fori_loop(1, nchunk, q_step, 0)

    @pl.when(has_next)
    def _():
        kv_up.wait_send()
        x_up.wait_send()
        kv_dn.wait_recv()
        x_dn.wait_recv()
        kv[pl.ds(T + BLK, BLK), :] = kvhi[...]
        xbuf[pl.ds(T + EDGE, EDGE), :] = xhi[...]

    @pl.when(jnp.logical_not(has_next))
    def _():
        kv[pl.ds(T + BLK, BLK), :] = jnp.zeros((BLK, kv.shape[1]), BF16)
        xbuf[pl.ds(T + EDGE, EDGE), :] = jnp.zeros((EDGE, xw), F32)

    @pl.when(has_prev)
    def _():
        kv_dn.wait_send()
        x_dn.wait_send()
        kv_up.wait_recv()
        x_up.wait_recv()
        kv[pl.ds(0, BLK), :] = kvlo[...]
        xbuf[pl.ds(0, EDGE), :] = xlo[...]

    @pl.when(jnp.logical_not(has_prev))
    def _():
        kv[pl.ds(0, BLK), :] = jnp.zeros((BLK, kv.shape[1]), BF16)
        xbuf[pl.ds(0, EDGE), :] = jnp.zeros((EDGE, xw), F32)

    sq = (BLK, BLK)
    ri = lax.broadcasted_iota(jnp.int32, sq, 0)
    ci = lax.broadcasted_iota(jnp.int32, sq, 1)
    heads = inner_w // HEAD
    groups = state_w // STATE
    per_group = heads // groups
    gwid = per_group * HEAD
    low = low_half(sq)

    def spread(values, column):
        return jnp.broadcast_to(values[:, column : column + 1], sq)

    def paired(values, tile, direction):
        base = direction * heads + 2 * tile
        return jnp.where(low, spread(values, base), spread(values, base + 1))

    def state_step(b, carry):
        rows = pl.ds(pl.multiple_of(b * BLK, BLK), BLK)
        lower = jnp.where(ri >= ci, 1.0, 0.0).astype(F32)
        upper = jnp.where(ri <= ci, 1.0, 0.0).astype(F32)
        d = cb[rows, :]
        c = jnp.where(ci < heads, mm_hi(lower, d), mm_hi(upper, d))
        cb[rows, :] = c
        last = jnp.where(ci[:1] < heads, c[BLK - 1 : BLK, :], c[0:1, :])
        last8 = jnp.broadcast_to(last, (8, BLK))
        wide = jnp.exp(mm_hi(last8, expand[...]))
        dec[b, 0] = wide[:, :inner_w]
        dec[b, 1] = wide[:, inner_w:]
        load = st[rows, :] * jnp.exp(last - c)
        bt = []
        for s in range(xw - LANE, -1, -LANE):
            if s < inner_w:
                tap = taps_i[:, s : s + LANE].astype(F32)
            elif s < inner_w + state_w:
                tap = taps_b[:, s - inner_w : s - inner_w + LANE].astype(F32)
            else:
                o = s - inner_w - state_w
                tap = taps_c[:, o : o + LANE].astype(F32)
            win = xbuf[pl.ds(pl.multiple_of(b * BLK, BLK), BLK + 2 * EDGE), s : s + LANE]
            acc = jnp.zeros(sq, F32)
            for j in range(CONV):
                o = EDGE - CONV // 2 + j
                acc = acc + win[o : o + BLK] * tap[j : j + 1]
            a = silu(acc).astype(BF16)
            act[rows, s : s + LANE] = a
            if inner_w <= s < inner_w + state_w:
                bt.insert(0, a.astype(F32).T.astype(BF16))
            if s < inner_w:
                tile = s // LANE
                g = s // gwid
                af = a.astype(F32)
                for direction in range(2):
                    loaded = (af * paired(load, tile, direction)).astype(BF16)
                    gs[b, direction, :, s : s + LANE] = mm(bt[g], loaded)
        return carry

    lax.fori_loop(0, nb, state_step, 0)

    up = remote(chain_s.at[0], chain_r.at[0], sem_cs.at[0], sem_cr.at[0], idx + 1)
    dn = remote(chain_s.at[1], chain_r.at[1], sem_cs.at[1], sem_cr.at[1], idx - 1)

    def hop(direction, copy, first, has_source, has_target):
        @pl.when(has_source)
        def _():
            copy.wait_recv()

        @pl.when(has_target)
        def _():
            order = list(range(nb)) if direction == 0 else list(range(nb - 1, -1, -1))
            for s in range(0, inner_w, LANE):
                cols = slice(s, s + LANE)
                enter = jnp.where(
                    has_source, chain_r[direction, :, cols].astype(F32), start[direction, cols, :].T
                )
                total = enter
                for b in order:
                    total = total * dec[b, direction, 0:1, cols] + gs[b, direction, :, cols]
                chain_s[direction, :, cols] = total.astype(BF16)

    key_w = 3 * BLK
    aj = lax.broadcasted_iota(jnp.int32, (BLK, key_w), 1)
    ai = lax.broadcasted_iota(jnp.int32, (BLK, key_w), 0)
    reach = 2 * BLK
    kv_heads = kvw // HEAD
    q_per = (qw // HEAD) // kv_heads
    ones = jnp.ones((key_w, LANE), BF16)
    turn_up = (idx * nb) // n_sp
    turn_dn = ((n_sp - 1 - idx) * nb) // n_sp

    def attend(b, carry):
        @pl.when(b == turn_up)
        def _():
            hop(0, up, idx == 0, has_prev, has_next)

        @pl.when(b == turn_dn)
        def _():
            hop(1, dn, idx == n_sp - 1, has_next, has_prev)

        rows = pl.ds(pl.multiple_of(b * BLK, BLK), BLK)
        span = pl.ds(pl.multiple_of(b * BLK, BLK), key_w)
        lo = jnp.where((idx == 0) & (b == 0), BLK, 0)
        hi = jnp.where((idx == n_sp - 1) & (b == nb - 1), 2 * BLK - 1, key_w)
        valid = (aj >= jnp.maximum(ai, lo)) & (aj <= jnp.minimum(ai + reach, hi))
        for g in range(kv_heads):
            parts = []
            for t in range(q_per // 2):
                tile = g * (q_per // 2) + t
                q = qb[rows, tile * LANE : (tile + 1) * LANE]
                zero = jnp.zeros_like(q)
                parts += [jnp.where(low, q, zero), jnp.where(low, zero, q)]
            keys = kv[span, g * LANE : (g + 1) * LANE]
            vals = kv[span, (kv_heads + g) * LANE : (kv_heads + g + 1) * LANE]
            ext = jnp.concatenate([vals, ones], axis=1)
            s_all = mm_t(jnp.concatenate(parts, axis=0), keys)
            outs = []
            for r in range(q_per):
                s = jnp.where(valid, s_all[r * BLK : (r + 1) * BLK], -1e30)
                sk = sink[:, g * q_per + r : g * q_per + r + 1]
                m = jnp.maximum(jnp.max(s, axis=1, keepdims=True), sk)
                p = jnp.exp(s - m).astype(BF16)
                o = mm(p, ext)
                den = o[:, LANE:] + jnp.exp(sk - m)
                outs.append(o[:, :LANE] / den)
            for t in range(q_per // 2):
                tile = g * (q_per // 2) + t
                z[rows, tile * LANE : (tile + 1) * LANE] = jnp.where(
                    low, outs[2 * t], outs[2 * t + 1]
                ).astype(BF16)

        @pl.when((b == turn_up) & has_next)
        def _():
            up.start()

        @pl.when((b == turn_dn) & has_prev)
        def _():
            dn.start()

        return carry

    lax.fori_loop(0, nb, attend, 0)

    @pl.when(has_next)
    def _():
        up.wait_send()

    @pl.when(has_prev)
    def _():
        dn.wait_send()

    for direction in range(2):
        source = has_prev if direction == 0 else has_next
        order = list(range(nb)) if direction == 0 else list(range(nb - 1, -1, -1))
        for s in range(0, inner_w, LANE):
            cols = slice(s, s + LANE)
            total = jnp.where(
                source, chain_r[direction, :, cols].astype(F32), start[direction, cols, :].T
            )
            for b in order:
                sb[b, direction, :, cols] = total.astype(BF16)
                if b != order[-1]:
                    total = total * dec[b, direction, 0:1, cols] + gs[b, direction, :, cols]

    attn_w = qw

    def mix_block(b):
        rows = pl.ds(pl.multiple_of(b * BLK, BLK), BLK)
        c = cb[rows, :]
        step = st[rows, :]
        c_t = c.T
        step_t = step.T
        diag = ri == ci
        below = ri >= ci
        for g in range(groups):
            bm = act[rows, inner_w + g * STATE : inner_w + (g + 1) * STATE]
            cm = act[rows, inner_w + state_w + g * STATE : inner_w + state_w + (g + 1) * STATE]
            scores = mm_t(cm, bm)
            carried = [mm(cm, sb[b, d, :, g * gwid : (g + 1) * gwid]) for d in range(2)]
            gated = []
            for t in range(per_group // 2):
                tile = g * (per_group // 2) + t
                ws_ = []
                cols_f, cols_b = [], []
                for u in range(2):
                    h = 2 * tile + u
                    cf = spread(c, h)
                    cr = spread(c, heads + h)
                    cols_f.append(cf)
                    cols_b.append(cr)
                    arg = jnp.where(
                        below, cf - c_t[h : h + 1, :], cr - c_t[heads + h : heads + h + 1, :]
                    )
                    sf = step_t[h : h + 1, :]
                    sr = step_t[heads + h : heads + h + 1, :]
                    fac = jnp.where(diag, sf + sr, jnp.where(below, sf, sr))
                    ws_.append((scores * jnp.exp(arg) * fac).astype(BF16))
                y = mm(jnp.concatenate(ws_, axis=0), act[rows, tile * LANE : (tile + 1) * LANE])
                y = jnp.where(low, y[:BLK], y[BLK:])
                seg = slice(t * LANE, (t + 1) * LANE)
                y = y + carried[0][:, seg] * jnp.exp(jnp.where(low, cols_f[0], cols_f[1]))
                y = y + carried[1][:, seg] * jnp.exp(jnp.where(low, cols_b[0], cols_b[1]))
                gated.append(y * silu(gb[rows, tile * LANE : (tile + 1) * LANE].astype(F32)))
            total = sum(jnp.sum(v * v, axis=1, keepdims=True) for v in gated)
            inv = lax.rsqrt(total * (1.0 / gwid) + epsilon)
            for t, v in enumerate(gated):
                s = g * gwid + t * LANE
                z[rows, attn_w + s : attn_w + s + LANE] = (
                    v * inv * ggain[:, s : s + LANE]
                ).astype(BF16)

    for c in oc:
        c.wait()
    half_rows = T // 2
    steps = half_rows // ROWS
    width = wo.shape[1]

    def mix_rows(base):
        def one(k, carry):
            mix_block(base // BLK + k)
            return carry

        lax.fori_loop(0, ROWS // BLK, one, 0, unroll=True)

    copies = []
    for i in range(steps):
        base = peer * half_rows + i * ROWS
        mix_rows(base)
        zr = z[pl.ds(pl.multiple_of(base, ROWS), ROWS), :]
        for s in range(0, width, 512):
            psend[i * ROWS : (i + 1) * ROWS, s : s + 512] = mm(zr, wo[:, s : s + 512]).astype(BF16)
        copies.append(
            pltpu.make_async_remote_copy(
                src_ref=psend.at[pl.ds(i * ROWS, ROWS)],
                dst_ref=precv.at[pl.ds(i * ROWS, ROWS)],
                send_sem=sem_ps.at[i],
                recv_sem=sem_pr.at[i],
                device_id={"tp": peer},
                device_id_type=MESH,
            )
        )
        if i > 0:
            copies[i - 1].start()
    for i in range(steps):
        base = me * half_rows + i * ROWS
        mix_rows(base)
        if i == 0:
            copies[-1].start()
        zr = z[pl.ds(pl.multiple_of(base, ROWS), ROWS), :]
        for s in range(0, width, 512):
            part = mm(zr, wo[:, s : s + 512]).astype(BF16).astype(F32)
            if s == 0:
                copies[i].wait()
            got = precv[i * ROWS : (i + 1) * ROWS, s : s + 512].astype(F32)
            out_ref[i * ROWS : (i + 1) * ROWS, s : s + 512] = (part + got).astype(BF16)


def tables(tokens, count):
    lane = np.arange(LANE) % (HEAD // 2)
    frequency = rotary_base ** (-lane.astype(np.float64) / (HEAD // 2))
    inner = np.arange(tokens, dtype=np.float64)[:, None] * frequency[None, :]
    outer = np.arange(count, dtype=np.float64)[:, None] * tokens * frequency[None, :]
    return [f(a).astype(np.float32) for a in (inner, outer) for f in (np.cos, np.sin)]


def local(
    n_sp,
    inputs, mix_gain, w_query, w_key, w_value, query_gain, key_gain, sink_logit,
    w_inner, w_bmat, w_cmat, w_gate, w_step, conv_inner, conv_bmat, conv_cmat,
    step_bias, decay_rate, decay_offset, start_state, group_gain, w_out_attn, w_out_state,
):
    T, half = inputs.shape
    depth = w_query.shape[0]
    heads = w_step.shape[2]
    inner_w = w_inner.shape[1]
    state_w = w_bmat.shape[1]
    xw = inner_w + 2 * state_w
    kvw = w_key.shape[1]
    qw = w_query.shape[1]
    gw = w_gate.shape[1]
    width = w_out_attn.shape[1]
    nb = T // BLK
    nchunk = T // ROWS

    ws = w_step.reshape(depth, -1)
    offs = decay_offset.reshape(T, -1)
    start = start_state.reshape(2, inner_w, STATE)
    ct, sn, co, so = tables(T, n_sp)
    expand = np.zeros((LANE, 2 * inner_w), np.float32)
    for c in range(2 * heads):
        expand[c, c * HEAD : (c + 1) * HEAD] = 1.0
    any_spec = pl.BlockSpec(memory_space=pl.ANY)
    vm = pl.BlockSpec(memory_space=pltpu.VMEM)
    wcols = 2 * kvw + xw + qw + gw
    V = pltpu.VMEM
    dma = pltpu.SemaphoreType.DMA
    steps = T // 2 // ROWS
    scratch = [
        V((depth, wcols), BF16), V((depth, 2 * heads), BF16),
        V((w_out_attn.shape[0] + w_out_state.shape[0], width), BF16),
        V((T, half), BF16), V((T, half), BF16), V((T, 2 * half), BF16), V((T, LANE), F32),
        V((T + 2 * BLK, 4 * LANE), BF16), V((T + 2 * EDGE, xw), F32),
        V((T, qw), BF16), V((T, gw), BF16), V((T, LANE), F32), V((T, LANE), F32),
        V((T, xw), BF16),
        V((nb, 2, STATE, inner_w), F32), V((nb, 2, 8, inner_w), F32),
        V((nb, 2, STATE, inner_w), BF16),
        V((T, qw + inner_w), BF16),
        V((T // 2, width), BF16), V((T // 2, width), BF16),
        V((BLK, 4 * LANE), BF16), V((BLK, 4 * LANE), BF16),
        V((EDGE, xw), F32), V((EDGE, xw), F32),
        V((2, STATE, inner_w), BF16), V((2, STATE, inner_w), BF16),
        dma((10,)), dma((nchunk,)), dma((nchunk,)), dma((nchunk,)),
        dma((4,)), dma((4,)), dma((2,)), dma((2,)), dma((steps,)), dma((steps,)),
    ]
    return pl.pallas_call(
        functools.partial(kernel, n_sp=n_sp),
        out_shape=jax.ShapeDtypeStruct((T // 2, width), BF16),
        in_specs=[any_spec] * 11 + [vm] * 17,
        out_specs=vm,
        scratch_shapes=scratch,
        compiler_params=pltpu.CompilerParams(
            collective_id=0, has_side_effects=True, vmem_limit_bytes=67043328
        ),
        name="mixer",
    )(
        inputs, w_query, w_key, w_value, w_inner, w_bmat, w_cmat, w_gate, ws,
        w_out_attn, w_out_state,
        mix_gain.reshape(1, -1), query_gain.reshape(1, -1), key_gain.reshape(1, -1),
        sink_logit.reshape(1, -1), conv_inner, conv_bmat, conv_cmat, step_bias, decay_rate,
        offs, start,
        group_gain.reshape(1, -1), jnp.asarray(ct), jnp.asarray(sn), jnp.asarray(co),
        jnp.asarray(so), jnp.asarray(expand),
    )


def solution(mesh):
    return jax.shard_map(
        functools.partial(local, mesh.shape["sp"]),
        mesh=mesh,
        in_specs=(
            P(("fs", "sp"), "tp"),
            P(),
            P(None, "tp"),
            P(None, "tp"),
            P(None, "tp"),
            P(),
            P(),
            P("tp"),
            P(None, "tp"),
            P(None, "tp"),
            P(None, "tp"),
            P(None, "tp"),
            P(None, None, "tp"),
            P(None, "tp"),
            P(None, "tp"),
            P(None, "tp"),
            P(None, "tp"),
            P(None, "tp"),
            P("sp", None, "tp"),
            P("fs", "tp", None, None),
            P("tp"),
            P("tp", None),
            P("tp", None),
        ),
        out_specs=P(("fs", "sp", "tp"), None),
        check_vma=False,
    )
```
